32 devices in a mesh: row: 8 (over z, core), col: 4 (over y, x).
Axes of the slice: x: 2, y: 2, z: 4, core: 2. Of those that a mesh axis runs over, the one named last changes fastest.
Arguments:
- tokens: bfloat16 [4096, 2048], P('row'), may hold values from -6 to 6
- out_weight: bfloat16 [2048, 2048], P(None, 'col'), may hold values from -0.125 to 0.125
Outputs:
- mixed: bfloat16 [4096, 2048], P('row', 'col')
The draws below stay inside these ranges and needn't reach their ends.
All inputs are finite; a program needn't handle non-finite values.
Results may differ from the reference program's by a relative error of at most 0.001.
Values may be sent and summed in bfloat16 or wider, within the bound.
A program may use at most 64 MiB of HBM per device.

```python
import jax
import jax.numpy as jnp
from jax import lax

D = 2048
GROUPS = 4
GROUP_DIM = 512
LENGTH = 4096


def levels(own_key, extent, split, smallest, largest):
    def one(axis_at, parts):
        draws = jax.random.uniform(jax.random.fold_in(jax.random.fold_in(own_key, 6), axis_at), (parts,), jnp.float32, smallest / len(split), largest / len(split))
        return jnp.repeat(jnp.exp(draws), extent[axis_at] // parts).reshape((-1,) + (1,) * (len(extent) - axis_at - 1))

    factor_of = one(*split[0])
    for cut in split[1:]:
        factor_of = factor_of * one(*cut)
    return factor_of


def noise(rng, extent, width, bound, cuts=(), dtype=jnp.bfloat16):
    drawn = width * jax.random.normal(rng, extent, jnp.float32)
    if cuts:
        drawn = drawn * levels(rng, extent, cuts, -0.22, 0.18)
    return jnp.clip(drawn, -bound, bound).astype(dtype)


def setup_inputs(seed: int = 0) -> dict:
    keys = jax.random.split(jax.random.key(seed), 3)
    tokens = noise(keys[0], (LENGTH, D), 1.0, 6.0, ((0, 8),))
    out_weight = noise(keys[1], (D, D), D ** -0.5, 0.125, ((1, 4),))
    return {"tokens": tokens, "out_weight": out_weight}


def per_group(block):
    return jnp.fft.fft2(block, norm="ortho").real.astype(jnp.float32)


def reference(tokens, out_weight):
    grouped = tokens.astype(jnp.float32).reshape(LENGTH, GROUPS, GROUP_DIM)
    spectra = lax.map(per_group, jnp.moveaxis(grouped, 1, 0))
    spectral = jnp.moveaxis(spectra, 0, 1).reshape(LENGTH, D).astype(jnp.float32)
    mixed = jnp.dot(spectral, out_weight.astype(jnp.float32), precision=lax.Precision.HIGHEST, preferred_element_type=jnp.float32)
    return mixed.astype(jnp.bfloat16)
```

```python
import math

import functools

import jax
import jax.numpy as jnp
import numpy as np
from jax import lax
from jax.experimental import pallas as pl
from jax.experimental.pallas import tpu as pltpu
from jax.sharding import PartitionSpec as P

GROUPS = 4
GROUP_DIM = 512


def angles(product, period):
    return (product % period).astype(jnp.float32) * (2.0 * math.pi / period)


def plain_dot(matrix, values):
    return jnp.dot(
        matrix, values, precision=lax.Precision.HIGHEST, preferred_element_type=jnp.float32
    )


def whole_transform(whole_rows, row_count, seg_rows, length):
    few_chans = whole_rows.shape[2]
    lattice = jnp.arange(row_count, dtype=jnp.int32)
    phases = angles(lattice[:, None] * lattice[None, :], row_count)
    cosine_table = jnp.cos(phases)
    sine_table = jnp.sin(phases)
    real_in = whole_rows[0].reshape(row_count, seg_rows * few_chans)
    imag_in = whole_rows[1].reshape(row_count, seg_rows * few_chans)
    first_re = (plain_dot(cosine_table, real_in) + plain_dot(sine_table, imag_in)).reshape(
        row_count, seg_rows, few_chans
    )
    first_im = (plain_dot(cosine_table, imag_in) - plain_dot(sine_table, real_in)).reshape(
        row_count, seg_rows, few_chans
    )
    inner = jnp.arange(seg_rows, dtype=jnp.int32)
    twist = angles(lattice[:, None] * inner[None, :], length)[:, :, None]
    twist_cos = jnp.cos(twist)
    twist_sin = jnp.sin(twist)
    turned_re = twist_cos * first_re + twist_sin * first_im
    turned_im = twist_cos * first_im - twist_sin * first_re
    folded_re = jnp.transpose(turned_re, (1, 0, 2)).reshape(seg_rows, row_count * few_chans)
    folded_im = jnp.transpose(turned_im, (1, 0, 2)).reshape(seg_rows, row_count * few_chans)
    seg_phases = angles(inner[:, None] * inner[None, :], seg_rows)
    real_part = plain_dot(jnp.cos(seg_phases), folded_re) + plain_dot(
        jnp.sin(seg_phases), folded_im
    )
    return real_part.reshape(length, few_chans)


def general_body(tokens, out_weight):
    seg_rows = tokens.shape[0]
    col_width = out_weight.shape[1]
    row_count = lax.axis_size("row")
    length = seg_rows * row_count
    scaling = 1.0 / math.sqrt(length * GROUP_DIM)
    weight_wide = out_weight.astype(jnp.float32)
    lattice = jnp.arange(GROUP_DIM, dtype=jnp.int32)
    phases = angles(lattice[:, None] * lattice[None, :], GROUP_DIM)
    cosine_table = jnp.cos(phases) * scaling
    sine_table = jnp.sin(phases) * scaling
    folded_rows = []
    for group in range(GROUPS):
        group_rows = weight_wide[group * GROUP_DIM : (group + 1) * GROUP_DIM]
        folded_rows.append(
            jnp.concatenate(
                [plain_dot(cosine_table, group_rows), -plain_dot(sine_table, group_rows)], axis=1
            )
        )
    folded_map = jnp.concatenate(folded_rows, axis=0)
    spectrum = plain_dot(tokens.astype(jnp.float32), folded_map)
    stacked = jnp.stack([spectrum[:, :col_width], spectrum[:, col_width:]])
    whole_rows = lax.all_to_all(stacked, "row", split_axis=2, concat_axis=1, tiled=True)
    ordered = whole_transform(whole_rows, row_count, seg_rows, length)
    spectral = lax.all_to_all(
        ordered.astype(jnp.bfloat16), "row", split_axis=0, concat_axis=1, tiled=True
    )
    return spectral

RADIX = 8
HALF = 64
LANES = 128
EXTRA = 16
CODE = 84.0


def split_table(values):
    big = values.astype(jnp.bfloat16)
    return big, (values - big.astype(np.float64)).astype(jnp.bfloat16)


def tables(size, length):
    index = np.arange(size)
    phase = 2.0 * np.pi * ((index[:, None] * index[None, :]) % size) / size
    high, low = split_table(np.concatenate([np.cos(phase), np.sin(phase)], axis=0))
    turn = 2.0 * np.pi * (index[:, None] * np.arange(RADIX)[None, :]) / length
    twist = np.zeros((size, LANES), np.float32)
    twist[:, :RADIX] = np.cos(turn)
    twist[:, RADIX : 2 * RADIX] = np.sin(turn)
    small = np.arange(RADIX)
    eight = 2.0 * np.pi * ((small[:, None] * small[None, :]) % RADIX) / RADIX
    last = np.concatenate(
        [
            np.repeat(np.cos(eight)[:, :, None], HALF, axis=2),
            np.repeat(np.sin(eight)[:, :, None], HALF, axis=2),
        ],
        axis=2,
    ).astype(np.float32)
    inner = size // RADIX
    perm = np.zeros((size, size), np.float32)
    rows = np.arange(size)
    perm[rows, (rows % inner) * RADIX + rows // inner] = 1.0
    return high, low, twist, last, perm.astype(high.dtype)


def dot(a, b):
    return jnp.dot(a, b, preferred_element_type=jnp.float32)


def split(values):
    high = values.astype(jnp.bfloat16)
    return high, (values - high.astype(jnp.float32)).astype(jnp.bfloat16)


def peer_at(step, chip):
    upper = lax.rem(chip // 2 + 1 - step // 2, 2)
    lower = lax.rem(chip % 2 + (step + 1) // 2, 2)
    return upper * 2 + lower


def kernel(
    scaling,
    count,
    tok_ref,
    w_ref,
    high_ref,
    low_ref,
    twist_ref,
    last_ref,
    perm_ref,
    out_ref,
    tok_s,
    send_a,
    recv_a,
    zhigh,
    zlow,
    turned,
    send_b,
    recv_b,
    send_a_sem,
    recv_a_sem,
    send_b_sem,
    recv_b_sem,
):
    me = lax.axis_index("row")
    chip = me // 2
    chips = count // 2
    size = tok_ref.shape[0]
    groups = tok_ref.shape[1] // size
    inner = size // RADIX
    mid = size // 2
    barrier = pltpu.get_barrier_semaphore()
    for ahead in range(1, count):
        pl.semaphore_signal(
            barrier,
            inc=1,
            device_id={"row": lax.rem(me + ahead, count)},
            device_id_type=pl.DeviceIdType.MESH,
        )

    lane = lax.broadcasted_iota(jnp.int32, (1, LANES), 1)
    first = lane < HALF
    sign = jnp.where(first, 1.0, -1.0)

    for g in range(groups):
        cols = slice(g * size, (g + 1) * size)
        tok_s[:, cols] = dot(perm_ref[...], tok_ref[:, cols]).astype(jnp.bfloat16)

    def copy_a(target):
        return pltpu.make_async_remote_copy(
            src_ref=send_a.at[target],
            dst_ref=recv_a.at[me],
            send_sem=send_a_sem.at[target],
            recv_sem=recv_a_sem.at[me],
            device_id={"row": target},
            device_id_type=pl.DeviceIdType.MESH,
        )

    def copy_b(target):
        return pltpu.make_async_remote_copy(
            src_ref=send_b.at[target],
            dst_ref=recv_b.at[me],
            send_sem=send_b_sem.at[target],
            recv_sem=recv_b_sem.at[me],
            device_id={"row": target},
            device_id_type=pl.DeviceIdType.MESH,
        )

    pl.semaphore_wait(barrier, count - 1)

    @pl.loop(0, chips)
    def _(step):
        goal = peer_at(step, chip)
        cols = pl.ds(pl.multiple_of(goal * LANES, LANES), LANES)
        side = jnp.concatenate(
            [w_ref[g * size : (g + 1) * size, cols] for g in range(groups)], axis=1
        )
        folded = dot(high_ref[...], side) + dot(low_ref[...], side)
        total = None
        for g in range(groups):
            cosw = folded[:size, g * LANES : (g + 1) * LANES]
            sinw = -folded[size:, g * LANES : (g + 1) * LANES]
            pair = jnp.concatenate(
                [
                    jnp.where(first, cosw, pltpu.roll(sinw, HALF, 1)),
                    jnp.where(first, pltpu.roll(cosw, HALF, 1), sinw),
                ],
                axis=1,
            )
            high, low = split(pair)
            part = tok_s[:, g * size : (g + 1) * size]
            term = dot(part, high) + dot(part, low)
            total = term if total is None else total + term
        for core in range(2):
            target = goal * 2 + core
            block = total[:, core * LANES : (core + 1) * LANES]
            peak = jnp.max(jnp.abs(block), axis=1, keepdims=True)
            peak = jnp.max(peak, axis=0, keepdims=True)
            scale = jnp.broadcast_to(jnp.maximum(peak, 1e-30) * 1.0079, (EXTRA, LANES))
            scale = scale.astype(jnp.bfloat16)
            factor = CODE / scale[0:1].astype(jnp.float32)
            code = jnp.exp(jnp.abs(block) * factor) - 1.0
            code = jnp.where(block < 0.0, -code, code).astype(jnp.bfloat16)

            @pl.when(target != me)
            def _():
                send_a[target, :size] = code
                send_a[target, size:] = scale
                copy_a(target).start()

            @pl.when(target == me)
            def _():
                recv_a[target, :size] = code
                recv_a[target, size:] = scale

    @pl.loop(0, count)
    def _(at):
        source = peer_at(chips - 1 - at // 2, chip) * 2 + at % 2

        @pl.when(source != me)
        def _():
            pltpu.make_async_remote_copy(
                src_ref=send_a.at[source],
                dst_ref=recv_a.at[source],
                send_sem=send_a_sem.at[source],
                recv_sem=recv_a_sem.at[source],
                device_id={"row": source},
                device_id_type=pl.DeviceIdType.MESH,
            ).wait_recv()

        factor = recv_a[source, size:].astype(jnp.float32)[0:1] * (scaling / CODE)
        code = recv_a[source, :size].astype(jnp.float32)
        value = jnp.log(1.0 + jnp.abs(code)) * factor
        value = jnp.where(code < 0.0, -value, value)
        high, low = split(value)
        rows = pl.ds(pl.multiple_of(source * inner, inner), inner)
        for t in range(RADIX):
            zhigh[rows, t * LANES : (t + 1) * LANES] = high[t * inner : (t + 1) * inner]
            zlow[rows, t * LANES : (t + 1) * LANES] = low[t * inner : (t + 1) * inner]

    for pair in range(RADIX // 2):
        cols = slice(pair * 2 * LANES, (pair + 1) * 2 * LANES)
        found = dot(high_ref[...], zhigh[:, cols])
        found += dot(high_ref[...], zlow[:, cols])
        found += dot(low_ref[...], zhigh[:, cols])
        for half in range(2):
            t = pair * 2 + half
            cosz = found[:size, half * LANES : (half + 1) * LANES]
            sinz = found[size:, half * LANES : (half + 1) * LANES]
            whole = cosz + sign * pltpu.roll(sinz, HALF, 1)
            if t:
                whole = twist_ref[:, t : t + 1] * whole + (
                    twist_ref[:, RADIX + t : RADIX + t + 1] * sign
                ) * pltpu.roll(whole, HALF, 1)
            turned[t] = whole

    @pl.loop(0, count)
    def _(at):
        target = peer_at(at // 2, chip) * 2 + at % 2
        weights = last_ref[target]
        rows_at = 32
        for chunk in range(mid // rows_at):
            upper = slice(chunk * rows_at, (chunk + 1) * rows_at)
            under = slice(mid + chunk * rows_at, mid + (chunk + 1) * rows_at)
            top = weights[0:1] * turned[0, upper]
            bottom = weights[0:1] * turned[0, under]
            for t in range(1, RADIX):
                top += weights[t : t + 1] * turned[t, upper]
                bottom += weights[t : t + 1] * turned[t, under]
            packed = jnp.where(first, top, bottom) + pltpu.roll(
                jnp.where(first, bottom, top), HALF, 1
            )
            packed = packed.astype(jnp.bfloat16)
            send_b[target, upper] = packed

        @pl.when(target != me)
        def _():
            copy_b(target).start()

    recv_b[me] = send_b[me]

    for at in range(chips):
        goal = peer_at(chips - 1 - at, chip)
        for core in range(2):
            source = goal * 2 + core

            @pl.when(source != me)
            def _():
                pltpu.make_async_remote_copy(
                    src_ref=send_b.at[source],
                    dst_ref=recv_b.at[source],
                    send_sem=send_b_sem.at[source],
                    recv_sem=recv_b_sem.at[source],
                    device_id={"row": source},
                    device_id_type=pl.DeviceIdType.MESH,
                ).wait_recv()

        left = recv_b[goal * 2].astype(jnp.float32)
        right = recv_b[goal * 2 + 1].astype(jnp.float32)
        cols = pl.ds(pl.multiple_of(goal * LANES, LANES), LANES)
        out_ref[:mid, cols] = jnp.where(first, left, pltpu.roll(right, HALF, 1)).astype(
            jnp.bfloat16
        )
        out_ref[mid:, cols] = jnp.where(first, pltpu.roll(left, HALF, 1), right).astype(
            jnp.bfloat16
        )

    @pl.loop(1, count)
    def _(ahead):
        target = lax.rem(me + ahead, count)
        copy_a(target).wait_send()
        copy_b(target).wait_send()


def kernel_body(count, tokens, out_weight):
    size = tokens.shape[0]
    length = size * count
    scaling = 1.0 / math.sqrt(length * GROUP_DIM)
    vmem = pl.BlockSpec(memory_space=pltpu.VMEM)
    consts = [jnp.asarray(table) for table in tables(size, length)]
    return pl.pallas_call(
        functools.partial(kernel, scaling, count),
        out_shape=jax.ShapeDtypeStruct((size, out_weight.shape[1]), jnp.bfloat16),
        in_specs=[vmem] * (2 + len(consts)),
        out_specs=vmem,
        scratch_shapes=[
            pltpu.VMEM(tokens.shape, jnp.bfloat16),
            pltpu.VMEM((count, size + EXTRA, LANES), jnp.bfloat16),
            pltpu.VMEM((count, size + EXTRA, LANES), jnp.bfloat16),
            pltpu.VMEM((size, RADIX * LANES), jnp.bfloat16),
            pltpu.VMEM((size, RADIX * LANES), jnp.bfloat16),
            pltpu.VMEM((RADIX, size, LANES), jnp.float32),
            pltpu.VMEM((count, size // 2, LANES), jnp.bfloat16),
            pltpu.VMEM((count, size // 2, LANES), jnp.bfloat16),
            pltpu.SemaphoreType.DMA((count,)),
            pltpu.SemaphoreType.DMA((count,)),
            pltpu.SemaphoreType.DMA((count,)),
            pltpu.SemaphoreType.DMA((count,)),
        ],
        compiler_params=pltpu.CompilerParams(
            collective_id=0, has_side_effects=True, vmem_limit_bytes=60 * 1024 * 1024
        ),
    )(tokens, out_weight, *consts)


def body(tokens, out_weight):
    size = tokens.shape[0]
    count = lax.axis_size("row")
    fits = (
        count == RADIX
        and size == GROUP_DIM
        and tokens.shape[1] == GROUPS * GROUP_DIM
        and out_weight.shape[1] == count * HALF
    )
    if fits:
        return kernel_body(count, tokens, out_weight)
    return general_body(tokens, out_weight)


def solution(mesh):
    placed = (P("row", None), P(None, "col"))
    return jax.shard_map(
        body, mesh=mesh, in_specs=placed, out_specs=P("row", "col"), check_vma=False
    )
```

```python
import math

import functools

import jax
import jax.numpy as jnp
import numpy as np
from jax import lax
from jax.experimental import pallas as pl
from jax.experimental.pallas import tpu as pltpu
from jax.sharding import PartitionSpec as P

GROUPS = 4
GROUP_DIM = 512


def angles(product, period):
    return (product % period).astype(jnp.float32) * (2.0 * math.pi / period)


def plain_dot(matrix, values):
    return jnp.dot(
        matrix, values, precision=lax.Precision.HIGHEST, preferred_element_type=jnp.float32
    )


def whole_transform(whole_rows, row_count, seg_rows, length):
    few_chans = whole_rows.shape[2]
    lattice = jnp.arange(row_count, dtype=jnp.int32)
    phases = angles(lattice[:, None] * lattice[None, :], row_count)
    cosine_table = jnp.cos(phases)
    sine_table = jnp.sin(phases)
    real_in = whole_rows[0].reshape(row_count, seg_rows * few_chans)
    imag_in = whole_rows[1].reshape(row_count, seg_rows * few_chans)
    first_re = (plain_dot(cosine_table, real_in) + plain_dot(sine_table, imag_in)).reshape(
        row_count, seg_rows, few_chans
    )
    first_im = (plain_dot(cosine_table, imag_in) - plain_dot(sine_table, real_in)).reshape(
        row_count, seg_rows, few_chans
    )
    inner = jnp.arange(seg_rows, dtype=jnp.int32)
    twist = angles(lattice[:, None] * inner[None, :], length)[:, :, None]
    twist_cos = jnp.cos(twist)
    twist_sin = jnp.sin(twist)
    turned_re = twist_cos * first_re + twist_sin * first_im
    turned_im = twist_cos * first_im - twist_sin * first_re
    folded_re = jnp.transpose(turned_re, (1, 0, 2)).reshape(seg_rows, row_count * few_chans)
    folded_im = jnp.transpose(turned_im, (1, 0, 2)).reshape(seg_rows, row_count * few_chans)
    seg_phases = angles(inner[:, None] * inner[None, :], seg_rows)
    real_part = plain_dot(jnp.cos(seg_phases), folded_re) + plain_dot(
        jnp.sin(seg_phases), folded_im
    )
    return real_part.reshape(length, few_chans)


def general_body(tokens, out_weight):
    seg_rows = tokens.shape[0]
    col_width = out_weight.shape[1]
    row_count = lax.axis_size("row")
    length = seg_rows * row_count
    scaling = 1.0 / math.sqrt(length * GROUP_DIM)
    weight_wide = out_weight.astype(jnp.float32)
    lattice = jnp.arange(GROUP_DIM, dtype=jnp.int32)
    phases = angles(lattice[:, None] * lattice[None, :], GROUP_DIM)
    cosine_table = jnp.cos(phases) * scaling
    sine_table = jnp.sin(phases) * scaling
    folded_rows = []
    for group in range(GROUPS):
        group_rows = weight_wide[group * GROUP_DIM : (group + 1) * GROUP_DIM]
        folded_rows.append(
            jnp.concatenate(
                [plain_dot(cosine_table, group_rows), -plain_dot(sine_table, group_rows)], axis=1
            )
        )
    folded_map = jnp.concatenate(folded_rows, axis=0)
    spectrum = plain_dot(tokens.astype(jnp.float32), folded_map)
    stacked = jnp.stack([spectrum[:, :col_width], spectrum[:, col_width:]])
    whole_rows = lax.all_to_all(stacked, "row", split_axis=2, concat_axis=1, tiled=True)
    ordered = whole_transform(whole_rows, row_count, seg_rows, length)
    spectral = lax.all_to_all(
        ordered.astype(jnp.bfloat16), "row", split_axis=0, concat_axis=1, tiled=True
    )
    return spectral

RADIX = 8
HALF = 64
LANES = 128
EXTRA = 16
PARTS = 4
CODE = 84.0


def split_table(values):
    big = values.astype(jnp.bfloat16)
    return big, (values - big.astype(np.float64)).astype(jnp.bfloat16)


def tables(size, length):
    index = np.arange(size)
    phase = 2.0 * np.pi * ((index[:, None] * index[None, :]) % size) / size
    high, low = split_table(np.concatenate([np.cos(phase), np.sin(phase)], axis=0))
    turn = 2.0 * np.pi * (index[:, None] * np.arange(RADIX)[None, :]) / length
    twist = np.zeros((size, LANES), np.float32)
    twist[:, :RADIX] = np.cos(turn)
    twist[:, RADIX : 2 * RADIX] = np.sin(turn)
    small = np.arange(RADIX)
    eight = 2.0 * np.pi * ((small[:, None] * small[None, :]) % RADIX) / RADIX
    last = np.concatenate(
        [
            np.repeat(np.cos(eight)[:, :, None], HALF, axis=2),
            np.repeat(np.sin(eight)[:, :, None], HALF, axis=2),
        ],
        axis=2,
    ).astype(np.float32)
    return high, low, twist, last


def dot(a, b):
    return jnp.dot(a, b, preferred_element_type=jnp.float32)


def split(values):
    high = values.astype(jnp.bfloat16)
    return high, (values - high.astype(jnp.float32)).astype(jnp.bfloat16)


def peer_at(step, chip):
    upper = chip // 2
    folded = chip + upper * (3 - 2 * chip)
    place = lax.rem(step + 1 + folded, 4)
    goal = place + place // 2 - 2 * (place // 3)
    return goal + upper * (3 - 2 * goal)


def kernel(
    scaling,
    count,
    tok_hbm,
    w_hbm,
    high_hbm,
    low_hbm,
    twist_ref,
    last_ref,
    out_ref,
    tok_ref,
    w_ref,
    high_ref,
    low_ref,
    tok_s,
    send_a,
    recv_a,
    zhigh,
    zlow,
    turned,
    send_b,
    recv_b,
    load_sem,
    send_a_sem,
    recv_a_sem,
    send_b_sem,
    recv_b_sem,
):
    me = lax.axis_index("row")
    chip = me // 2
    chips = count // 2
    size = tok_ref.shape[0]
    groups = tok_ref.shape[1] // size
    inner = size // RADIX
    mid = size // 2
    part_rows = size // PARTS
    loads = []
    for at, (source, target) in enumerate(
        [(high_hbm, high_ref), (w_hbm, w_ref), (low_hbm, low_ref), (tok_hbm, tok_ref)]
    ):
        loads.append(pltpu.make_async_copy(source, target, load_sem.at[at]))
        loads[-1].start()
    barrier = pltpu.get_barrier_semaphore()
    for ahead in range(1, count):
        pl.semaphore_signal(
            barrier,
            inc=1,
            device_id={"row": lax.rem(me + ahead, count)},
            device_id_type=pl.DeviceIdType.MESH,
        )

    lane = lax.broadcasted_iota(jnp.int32, (1, LANES), 1)
    first = lane < HALF
    sign = jnp.where(first, 1.0, -1.0)

    def copy_a(part, target):
        return pltpu.make_async_remote_copy(
            src_ref=send_a.at[part, target],
            dst_ref=recv_a.at[part, me],
            send_sem=send_a_sem.at[part, target],
            recv_sem=recv_a_sem.at[part, me],
            device_id={"row": target},
            device_id_type=pl.DeviceIdType.MESH,
        )

    def copy_b(target):
        return pltpu.make_async_remote_copy(
            src_ref=send_b.at[target],
            dst_ref=recv_b.at[me],
            send_sem=send_b_sem.at[target],
            recv_sem=recv_b_sem.at[me],
            device_id={"row": target},
            device_id_type=pl.DeviceIdType.MESH,
        )

    for load in loads[:3]:
        load.wait()

    @pl.loop(0, chips)
    def _(step):
        goal = peer_at(step, chip)
        cols = pl.ds(pl.multiple_of(goal * LANES, LANES), LANES)
        side = jnp.concatenate(
            [w_ref[g * size : (g + 1) * size, cols] for g in range(groups)], axis=1
        )
        folded = dot(high_ref[...], side) + dot(low_ref[...], side)

        @pl.when(step == 0)
        def _():
            loads[3].wait()
            spot = lax.broadcasted_iota(jnp.int32, (size, size), 0)
            spot = (spot % inner) * RADIX + spot // inner
            place = lax.broadcasted_iota(jnp.int32, (size, size), 1)
            perm = jnp.where(spot == place, 1.0, 0.0).astype(jnp.bfloat16)
            for g in range(groups):
                span = slice(g * size, (g + 1) * size)
                tok_s[:, span] = dot(perm, tok_ref[:, span]).astype(jnp.bfloat16)

        total = None
        for g in range(groups):
            cosw = folded[:size, g * LANES : (g + 1) * LANES]
            sinw = -folded[size:, g * LANES : (g + 1) * LANES]
            pair = jnp.concatenate(
                [
                    jnp.where(first, cosw, pltpu.roll(sinw, HALF, 1)),
                    jnp.where(first, pltpu.roll(cosw, HALF, 1), sinw),
                ],
                axis=1,
            )
            high, low = split(pair)
            part = tok_s[:, g * size : (g + 1) * size]
            term = dot(part, high) + dot(part, low)
            total = term if total is None else total + term
        for core in range(2):
            target = goal * 2 + core
            block = total[:, core * LANES : (core + 1) * LANES]
            peak = jnp.max(jnp.abs(block), axis=1, keepdims=True)
            peak = jnp.max(peak, axis=0, keepdims=True)
            scale = jnp.broadcast_to(jnp.maximum(peak, 1e-30) * 1.0079, (EXTRA, LANES))
            scale = scale.astype(jnp.bfloat16)
            factor = CODE / scale[0:1].astype(jnp.float32)
            code = jnp.exp(jnp.abs(block) * factor) - 1.0
            code = jnp.where(block < 0.0, -code, code).astype(jnp.bfloat16)
            for part in range(PARTS):
                rows = slice(part * part_rows, (part + 1) * part_rows)
                send_a[part, target, :part_rows] = code[rows]
                send_a[part, target, part_rows:] = scale

        def ship(parts, steps):
            for part in parts:
                for at in steps:
                    for core in range(2):
                        copy_a(part, peer_at(at, chip) * 2 + core).start()

        half = range(PARTS // 2)
        rest = range(PARTS // 2, PARTS)

        @pl.when(step == 0)
        def _():
            pl.semaphore_wait(barrier, count - 1)
            ship(half, [0])

        @pl.when(step == 1)
        def _():
            ship(half, [1])

        @pl.when(step == 2)
        def _():
            ship(half, [2])
            ship(rest, [0, 1, 2])

        @pl.when(step == chips - 1)
        def _():
            for part in range(PARTS):
                copy_a(part, chip * 2 + (1 - me % 2)).start()
                recv_a[part, me] = send_a[part, me]

    for pair in range(RADIX // 2):

        @pl.loop(0, count)
        def _(at):
            source = peer_at(chips - 1 - at // 2, chip) * 2 + at % 2

            @pl.when(source != me)
            def _():
                pltpu.make_async_remote_copy(
                    src_ref=send_a.at[pair, source],
                    dst_ref=recv_a.at[pair, source],
                    send_sem=send_a_sem.at[pair, source],
                    recv_sem=recv_a_sem.at[pair, source],
                    device_id={"row": source},
                    device_id_type=pl.DeviceIdType.MESH,
                ).wait_recv()

            factor = recv_a[pair, source, part_rows:].astype(jnp.float32)[0:1]
            factor = factor * (scaling / CODE)
            code = recv_a[pair, source, :part_rows].astype(jnp.float32)
            value = jnp.log(1.0 + jnp.abs(code)) * factor
            value = jnp.where(code < 0.0, -value, value)
            high, low = split(value)
            rows = pl.ds(pl.multiple_of(source * inner, inner), inner)
            for half in range(2):
                span = slice((pair * 2 + half) * LANES, (pair * 2 + half + 1) * LANES)
                zhigh[rows, span] = high[half * inner : (half + 1) * inner]
                zlow[rows, span] = low[half * inner : (half + 1) * inner]

        cols = slice(pair * 2 * LANES, (pair + 1) * 2 * LANES)
        found = dot(high_ref[...], zhigh[:, cols])
        found += dot(high_ref[...], zlow[:, cols])
        found += dot(low_ref[...], zhigh[:, cols])
        for half in range(2):
            t = pair * 2 + half
            cosz = found[:size, half * LANES : (half + 1) * LANES]
            sinz = found[size:, half * LANES : (half + 1) * LANES]
            whole = cosz + sign * pltpu.roll(sinz, HALF, 1)
            if t:
                whole = twist_ref[:, t : t + 1] * whole + (
                    twist_ref[:, RADIX + t : RADIX + t + 1] * sign
                ) * pltpu.roll(whole, HALF, 1)
            turned[t] = whole

    @pl.loop(0, count)
    def _(at):
        target = peer_at(at // 2, chip) * 2 + at % 2
        weights = last_ref[target]
        rows_at = 32
        for chunk in range(mid // rows_at):
            upper = slice(chunk * rows_at, (chunk + 1) * rows_at)
            under = slice(mid + chunk * rows_at, mid + (chunk + 1) * rows_at)
            top = weights[0:1] * turned[0, upper]
            bottom = weights[0:1] * turned[0, under]
            for t in range(1, RADIX):
                top += weights[t : t + 1] * turned[t, upper]
                bottom += weights[t : t + 1] * turned[t, under]
            packed = jnp.where(first, top, bottom) + pltpu.roll(
                jnp.where(first, bottom, top), HALF, 1
            )
            packed = packed.astype(jnp.bfloat16)
            send_b[target, upper] = packed

        @pl.when(target != me)
        def _():
            copy_b(target).start()

    recv_b[me] = send_b[me]

    for at in range(chips):
        goal = peer_at(chips - 1 - at, chip)
        for core in range(2):
            source = goal * 2 + core

            @pl.when(source != me)
            def _():
                pltpu.make_async_remote_copy(
                    src_ref=send_b.at[source],
                    dst_ref=recv_b.at[source],
                    send_sem=send_b_sem.at[source],
                    recv_sem=recv_b_sem.at[source],
                    device_id={"row": source},
                    device_id_type=pl.DeviceIdType.MESH,
                ).wait_recv()

        left = recv_b[goal * 2].astype(jnp.float32)
        right = recv_b[goal * 2 + 1].astype(jnp.float32)
        cols = pl.ds(pl.multiple_of(goal * LANES, LANES), LANES)
        out_ref[:mid, cols] = jnp.where(first, left, pltpu.roll(right, HALF, 1)).astype(
            jnp.bfloat16
        )
        out_ref[mid:, cols] = jnp.where(first, pltpu.roll(left, HALF, 1), right).astype(
            jnp.bfloat16
        )

    @pl.loop(1, count)
    def _(ahead):
        target = lax.rem(me + ahead, count)
        for part in range(PARTS):
            copy_a(part, target).wait_send()
        copy_b(target).wait_send()


def kernel_body(count, tokens, out_weight):
    size = tokens.shape[0]
    length = size * count
    scaling = 1.0 / math.sqrt(length * GROUP_DIM)
    vmem = pl.BlockSpec(memory_space=pltpu.VMEM)
    consts = [jnp.asarray(table) for table in tables(size, length)]
    return pl.pallas_call(
        functools.partial(kernel, scaling, count),
        out_shape=jax.ShapeDtypeStruct((size, out_weight.shape[1]), jnp.bfloat16),
        in_specs=[pl.BlockSpec(memory_space=pl.ANY)] * 4 + [vmem] * 2,
        out_specs=vmem,
        scratch_shapes=[
            pltpu.VMEM(tokens.shape, jnp.bfloat16),
            pltpu.VMEM(out_weight.shape, jnp.bfloat16),
            pltpu.VMEM((2 * size, size), jnp.bfloat16),
            pltpu.VMEM((2 * size, size), jnp.bfloat16),
            pltpu.VMEM(tokens.shape, jnp.bfloat16),
            pltpu.VMEM((PARTS, count, size // PARTS + EXTRA, LANES), jnp.bfloat16),
            pltpu.VMEM((PARTS, count, size // PARTS + EXTRA, LANES), jnp.bfloat16),
            pltpu.VMEM((size, RADIX * LANES), jnp.bfloat16),
            pltpu.VMEM((size, RADIX * LANES), jnp.bfloat16),
            pltpu.VMEM((RADIX, size, LANES), jnp.float32),
            pltpu.VMEM((count, size // 2, LANES), jnp.bfloat16),
            pltpu.VMEM((count, size // 2, LANES), jnp.bfloat16),
            pltpu.SemaphoreType.DMA((4,)),
            pltpu.SemaphoreType.DMA((PARTS, count)),
            pltpu.SemaphoreType.DMA((PARTS, count)),
            pltpu.SemaphoreType.DMA((count,)),
            pltpu.SemaphoreType.DMA((count,)),
        ],
        compiler_params=pltpu.CompilerParams(
            collective_id=0, has_side_effects=True, vmem_limit_bytes=60 * 1024 * 1024
        ),
    )(tokens, out_weight, *consts)


def body(tokens, out_weight):
    size = tokens.shape[0]
    count = lax.axis_size("row")
    fits = (
        count == RADIX
        and size == GROUP_DIM
        and tokens.shape[1] == GROUPS * GROUP_DIM
        and out_weight.shape[1] == count * HALF
    )
    if fits:
        return kernel_body(count, tokens, out_weight)
    return general_body(tokens, out_weight)


def solution(mesh):
    placed = (P("row", None), P(None, "col"))
    return jax.shard_map(
        body, mesh=mesh, in_specs=placed, out_specs=P("row", "col"), check_vma=False
    )
```

```python
import math

import functools

import jax
import jax.numpy as jnp
import numpy as np
from jax import lax
from jax.experimental import pallas as pl
from jax.experimental.pallas import tpu as pltpu
from jax.sharding import PartitionSpec as P

GROUPS = 4
GROUP_DIM = 512


def angles(product, period):
    return (product % period).astype(jnp.float32) * (2.0 * math.pi / period)


def plain_dot(matrix, values):
    return jnp.dot(
        matrix, values, precision=lax.Precision.HIGHEST, preferred_element_type=jnp.float32
    )


def whole_transform(whole_rows, row_count, seg_rows, length):
    few_chans = whole_rows.shape[2]
    lattice = jnp.arange(row_count, dtype=jnp.int32)
    phases = angles(lattice[:, None] * lattice[None, :], row_count)
    cosine_table = jnp.cos(phases)
    sine_table = jnp.sin(phases)
    real_in = whole_rows[0].reshape(row_count, seg_rows * few_chans)
    imag_in = whole_rows[1].reshape(row_count, seg_rows * few_chans)
    first_re = (plain_dot(cosine_table, real_in) + plain_dot(sine_table, imag_in)).reshape(
        row_count, seg_rows, few_chans
    )
    first_im = (plain_dot(cosine_table, imag_in) - plain_dot(sine_table, real_in)).reshape(
        row_count, seg_rows, few_chans
    )
    inner = jnp.arange(seg_rows, dtype=jnp.int32)
    twist = angles(lattice[:, None] * inner[None, :], length)[:, :, None]
    twist_cos = jnp.cos(twist)
    twist_sin = jnp.sin(twist)
    turned_re = twist_cos * first_re + twist_sin * first_im
    turned_im = twist_cos * first_im - twist_sin * first_re
    folded_re = jnp.transpose(turned_re, (1, 0, 2)).reshape(seg_rows, row_count * few_chans)
    folded_im = jnp.transpose(turned_im, (1, 0, 2)).reshape(seg_rows, row_count * few_chans)
    seg_phases = angles(inner[:, None] * inner[None, :], seg_rows)
    real_part = plain_dot(jnp.cos(seg_phases), folded_re) + plain_dot(
        jnp.sin(seg_phases), folded_im
    )
    return real_part.reshape(length, few_chans)


def general_body(tokens, out_weight):
    seg_rows = tokens.shape[0]
    col_width = out_weight.shape[1]
    row_count = lax.axis_size("row")
    length = seg_rows * row_count
    scaling = 1.0 / math.sqrt(length * GROUP_DIM)
    weight_wide = out_weight.astype(jnp.float32)
    lattice = jnp.arange(GROUP_DIM, dtype=jnp.int32)
    phases = angles(lattice[:, None] * lattice[None, :], GROUP_DIM)
    cosine_table = jnp.cos(phases) * scaling
    sine_table = jnp.sin(phases) * scaling
    folded_rows = []
    for group in range(GROUPS):
        group_rows = weight_wide[group * GROUP_DIM : (group + 1) * GROUP_DIM]
        folded_rows.append(
            jnp.concatenate(
                [plain_dot(cosine_table, group_rows), -plain_dot(sine_table, group_rows)], axis=1
            )
        )
    folded_map = jnp.concatenate(folded_rows, axis=0)
    spectrum = plain_dot(tokens.astype(jnp.float32), folded_map)
    stacked = jnp.stack([spectrum[:, :col_width], spectrum[:, col_width:]])
    whole_rows = lax.all_to_all(stacked, "row", split_axis=2, concat_axis=1, tiled=True)
    ordered = whole_transform(whole_rows, row_count, seg_rows, length)
    spectral = lax.all_to_all(
        ordered.astype(jnp.bfloat16), "row", split_axis=0, concat_axis=1, tiled=True
    )
    return spectral

RADIX = 8
HALF = 64
LANES = 128
EXTRA = 16
PARTS = 4
CODE = 84.0


def split_table(values):
    big = values.astype(jnp.bfloat16)
    return big, (values - big.astype(np.float64)).astype(jnp.bfloat16)


def tables(size, length):
    index = np.arange(size)
    phase = 2.0 * np.pi * ((index[:, None] * index[None, :]) % size) / size
    high, low = split_table(np.concatenate([np.cos(phase), np.sin(phase)], axis=0))
    turn = 2.0 * np.pi * (index[:, None] * np.arange(RADIX)[None, :]) / length
    twist = np.zeros((size, LANES), np.float32)
    twist[:, :RADIX] = np.cos(turn)
    twist[:, RADIX : 2 * RADIX] = np.sin(turn)
    small = np.arange(RADIX)
    eight = 2.0 * np.pi * ((small[:, None] * small[None, :]) % RADIX) / RADIX
    last = np.concatenate(
        [
            np.repeat(np.cos(eight)[:, :, None], HALF, axis=2),
            np.repeat(np.sin(eight)[:, :, None], HALF, axis=2),
        ],
        axis=2,
    ).astype(np.float32)
    return high, low, twist, last


def dot(a, b):
    return jnp.dot(a, b, preferred_element_type=jnp.float32)


def split(values):
    high = values.astype(jnp.bfloat16)
    return high, (values - high.astype(jnp.float32)).astype(jnp.bfloat16)


def peer_at(step, chip):
    upper = chip // 2
    folded = chip + upper * (3 - 2 * chip)
    place = lax.rem(step + 1 + folded, 4)
    goal = place + place // 2 - 2 * (place // 3)
    return goal + upper * (3 - 2 * goal)


def kernel(
    scaling,
    count,
    tok_hbm,
    w_hbm,
    high_hbm,
    low_hbm,
    twist_ref,
    last_ref,
    out_ref,
    tok_ref,
    w_ref,
    high_ref,
    low_ref,
    tok_s,
    send_a,
    recv_a,
    zhigh,
    zlow,
    turned,
    found_s,
    send_b,
    recv_b,
    load_sem,
    send_a_sem,
    recv_a_sem,
    send_b_sem,
    recv_b_sem,
):
    me = lax.axis_index("row")
    chip = me // 2
    chips = count // 2
    size = tok_ref.shape[0]
    groups = tok_ref.shape[1] // size
    inner = size // RADIX
    mid = size // 2
    part_rows = size // PARTS
    loads = []
    for at, (source, target) in enumerate(
        [(high_hbm, high_ref), (low_hbm, low_ref), (tok_hbm, tok_ref)]
    ):
        loads.append(pltpu.make_async_copy(source, target, load_sem.at[at]))

    def load_w(step):
        goal = peer_at(step, chip)
        cols = pl.ds(pl.multiple_of(goal * LANES, LANES), LANES)
        return pltpu.make_async_copy(
            w_hbm.at[:, cols], w_ref.at[:, cols], load_sem.at[3 + step]
        )

    load_w(0).start()
    for load in loads:
        load.start()
    for step in range(1, 4):
        load_w(step).start()
    barrier = pltpu.get_barrier_semaphore()
    for ahead in range(1, count):
        pl.semaphore_signal(
            barrier,
            inc=1,
            device_id={"row": lax.rem(me + ahead, count)},
            device_id_type=pl.DeviceIdType.MESH,
        )

    lane = lax.broadcasted_iota(jnp.int32, (1, LANES), 1)
    first = lane < HALF
    sign = jnp.where(first, 1.0, -1.0)

    def copy_a(part, target):
        return pltpu.make_async_remote_copy(
            src_ref=send_a.at[part, target],
            dst_ref=recv_a.at[part, me],
            send_sem=send_a_sem.at[part, target],
            recv_sem=recv_a_sem.at[part, me],
            device_id={"row": target},
            device_id_type=pl.DeviceIdType.MESH,
        )

    def copy_b(target):
        return pltpu.make_async_remote_copy(
            src_ref=send_b.at[target],
            dst_ref=recv_b.at[me],
            send_sem=send_b_sem.at[target],
            recv_sem=recv_b_sem.at[me],
            device_id={"row": target},
            device_id_type=pl.DeviceIdType.MESH,
        )

    for load in loads[:2]:
        load.wait()

    @pl.loop(0, chips)
    def _(step):
        goal = peer_at(step, chip)
        cols = pl.ds(pl.multiple_of(goal * LANES, LANES), LANES)
        load_w(step).wait()
        side = jnp.concatenate(
            [w_ref[g * size : (g + 1) * size, cols] for g in range(groups)], axis=1
        )
        folded = dot(high_ref[...], side) + dot(low_ref[...], side)

        @pl.when(step == 0)
        def _():
            loads[2].wait()
            place = lax.broadcasted_iota(jnp.int32, (1, size), 1)
            place = (place % RADIX) * inner + place // RADIX
            spot = lax.broadcasted_iota(jnp.int32, (size, size), 0)
            perm = jnp.where(spot == place, 1.0, 0.0).astype(jnp.bfloat16)
            for g in range(groups):
                span = slice(g * size, (g + 1) * size)
                tok_s[:, span] = dot(perm, tok_ref[:, span]).astype(jnp.bfloat16)

        total = None
        for g in range(groups):
            cosw = folded[:size, g * LANES : (g + 1) * LANES]
            sinw = -folded[size:, g * LANES : (g + 1) * LANES]
            pair = jnp.concatenate(
                [
                    jnp.where(first, cosw, pltpu.roll(sinw, HALF, 1)),
                    jnp.where(first, pltpu.roll(cosw, HALF, 1), sinw),
                ],
                axis=1,
            )
            high, low = split(pair)
            part = tok_s[:, g * size : (g + 1) * size]
            term = dot(part, high) + dot(part, low)
            total = term if total is None else total + term
        for core in range(2):
            target = goal * 2 + core
            block = total[:, core * LANES : (core + 1) * LANES]
            peak = jnp.max(jnp.abs(block), axis=1, keepdims=True)
            peak = jnp.max(peak, axis=0, keepdims=True)
            scale = jnp.broadcast_to(jnp.maximum(peak, 1e-30) * 1.0079, (EXTRA, LANES))
            scale = scale.astype(jnp.bfloat16)
            factor = CODE / scale[0:1].astype(jnp.float32)
            code = jnp.exp(jnp.abs(block) * factor) - 1.0
            code = jnp.where(block < 0.0, -code, code).astype(jnp.bfloat16)
            for part in range(PARTS):
                rows = slice(part * part_rows, (part + 1) * part_rows)
                send_a[part, target, :part_rows] = code[rows]
                send_a[part, target, part_rows:] = scale

        def ship(parts, steps):
            for part in parts:
                for at in steps:
                    for core in range(2):
                        copy_a(part, peer_at(at, chip) * 2 + core).start()

        half = range(PARTS // 2)
        rest = range(PARTS // 2, PARTS)

        @pl.when(step == 0)
        def _():
            pl.semaphore_wait(barrier, count - 1)
            ship(half, [0])

        @pl.when(step == 1)
        def _():
            ship(half, [1])

        @pl.when(step == 2)
        def _():
            ship(half, [2])
            ship(rest, [0, 1, 2])

        @pl.when(step == chips - 1)
        def _():
            for part in range(PARTS):
                copy_a(part, chip * 2 + (1 - me % 2)).start()
                recv_a[part, me] = send_a[part, me]

    for pair in range(RADIX // 2):

        def take(at, base):
            source = base + at

            @pl.when(source != me)
            def _():
                pltpu.make_async_remote_copy(
                    src_ref=send_a.at[pair, source],
                    dst_ref=recv_a.at[pair, source],
                    send_sem=send_a_sem.at[pair, source],
                    recv_sem=recv_a_sem.at[pair, source],
                    device_id={"row": source},
                    device_id_type=pl.DeviceIdType.MESH,
                ).wait_recv()

            factor = recv_a[pair, source, part_rows:].astype(jnp.float32)[0:1]
            factor = factor * (scaling / CODE)
            code = recv_a[pair, source, :part_rows].astype(jnp.float32)
            value = jnp.log(1.0 + jnp.abs(code)) * factor
            value = jnp.where(code < 0.0, -value, value)
            high, low = split(value)
            rows = pl.ds(pl.multiple_of(source * inner, inner), inner)
            for half in range(2):
                span = slice((pair * 2 + half) * LANES, (pair * 2 + half + 1) * LANES)
                zhigh[rows, span] = high[half * inner : (half + 1) * inner]
                zlow[rows, span] = low[half * inner : (half + 1) * inner]

        def near_or_far(base):
            pl.loop(0, count // 2)(lambda at: take(at, base))
            span = pl.ds(pl.multiple_of(base * inner, size // 2), size // 2)
            terms = dot(high_ref[:, span], zhigh[span, cols])
            terms += dot(high_ref[:, span], zlow[span, cols])
            return terms + dot(low_ref[:, span], zhigh[span, cols])

        cols = slice(pair * 2 * LANES, (pair + 1) * 2 * LANES)
        own = (me // (count // 2)) * (count // 2)
        found_s[...] = near_or_far(own)
        found = found_s[...] + near_or_far(count // 2 - own)
        for half in range(2):
            t = pair * 2 + half
            cosz = found[:size, half * LANES : (half + 1) * LANES]
            sinz = found[size:, half * LANES : (half + 1) * LANES]
            whole = cosz + sign * pltpu.roll(sinz, HALF, 1)
            if t:
                whole = twist_ref[:, t : t + 1] * whole + (
                    twist_ref[:, RADIX + t : RADIX + t + 1] * sign
                ) * pltpu.roll(whole, HALF, 1)
            turned[t] = whole

    @pl.loop(0, count)
    def _(at):
        target = peer_at(at // 2, chip) * 2 + at % 2
        weights = last_ref[target]
        rows_at = 32
        for chunk in range(mid // rows_at):
            upper = slice(chunk * rows_at, (chunk + 1) * rows_at)
            under = slice(mid + chunk * rows_at, mid + (chunk + 1) * rows_at)
            top = weights[0:1] * turned[0, upper]
            bottom = weights[0:1] * turned[0, under]
            for t in range(1, RADIX):
                top += weights[t : t + 1] * turned[t, upper]
                bottom += weights[t : t + 1] * turned[t, under]
            packed = jnp.where(first, top, bottom) + pltpu.roll(
                jnp.where(first, bottom, top), HALF, 1
            )
            packed = packed.astype(jnp.bfloat16)
            send_b[target, upper] = packed

        @pl.when(target != me)
        def _():
            copy_b(target).start()

    recv_b[me] = send_b[me]

    for at in range(chips):
        goal = peer_at(chips - 1 - at, chip)
        for core in range(2):
            source = goal * 2 + core

            @pl.when(source != me)
            def _():
                pltpu.make_async_remote_copy(
                    src_ref=send_b.at[source],
                    dst_ref=recv_b.at[source],
                    send_sem=send_b_sem.at[source],
                    recv_sem=recv_b_sem.at[source],
                    device_id={"row": source},
                    device_id_type=pl.DeviceIdType.MESH,
                ).wait_recv()

        left = recv_b[goal * 2].astype(jnp.float32)
        right = recv_b[goal * 2 + 1].astype(jnp.float32)
        cols = pl.ds(pl.multiple_of(goal * LANES, LANES), LANES)
        out_ref[:mid, cols] = jnp.where(first, left, pltpu.roll(right, HALF, 1)).astype(
            jnp.bfloat16
        )
        out_ref[mid:, cols] = jnp.where(first, pltpu.roll(left, HALF, 1), right).astype(
            jnp.bfloat16
        )

    @pl.loop(1, count)
    def _(ahead):
        target = lax.rem(me + ahead, count)
        for part in range(PARTS):
            copy_a(part, target).wait_send()
        copy_b(target).wait_send()


def kernel_body(count, tokens, out_weight):
    size = tokens.shape[0]
    length = size * count
    scaling = 1.0 / math.sqrt(length * GROUP_DIM)
    vmem = pl.BlockSpec(memory_space=pltpu.VMEM)
    consts = [jnp.asarray(table) for table in tables(size, length)]
    return pl.pallas_call(
        functools.partial(kernel, scaling, count),
        out_shape=jax.ShapeDtypeStruct((size, out_weight.shape[1]), jnp.bfloat16),
        in_specs=[pl.BlockSpec(memory_space=pl.ANY)] * 4 + [vmem] * 2,
        out_specs=vmem,
        scratch_shapes=[
            pltpu.VMEM(tokens.shape, jnp.bfloat16),
            pltpu.VMEM(out_weight.shape, jnp.bfloat16),
            pltpu.VMEM((2 * size, size), jnp.bfloat16),
            pltpu.VMEM((2 * size, size), jnp.bfloat16),
            pltpu.VMEM(tokens.shape, jnp.bfloat16),
            pltpu.VMEM((PARTS, count, size // PARTS + EXTRA, LANES), jnp.bfloat16),
            pltpu.VMEM((PARTS, count, size // PARTS + EXTRA, LANES), jnp.bfloat16),
            pltpu.VMEM((size, RADIX * LANES), jnp.bfloat16),
            pltpu.VMEM((size, RADIX * LANES), jnp.bfloat16),
            pltpu.VMEM((RADIX, size, LANES), jnp.float32),
            pltpu.VMEM((2 * size, 2 * LANES), jnp.float32),
            pltpu.VMEM((count, size // 2, LANES), jnp.bfloat16),
            pltpu.VMEM((count, size // 2, LANES), jnp.bfloat16),
            pltpu.SemaphoreType.DMA((7,)),
            pltpu.SemaphoreType.DMA((PARTS, count)),
            pltpu.SemaphoreType.DMA((PARTS, count)),
            pltpu.SemaphoreType.DMA((count,)),
            pltpu.SemaphoreType.DMA((count,)),
        ],
        compiler_params=pltpu.CompilerParams(
            collective_id=0, has_side_effects=True, vmem_limit_bytes=60 * 1024 * 1024
        ),
    )(tokens, out_weight, *consts)


def body(tokens, out_weight):
    size = tokens.shape[0]
    count = lax.axis_size("row")
    fits = (
        count == RADIX
        and size == GROUP_DIM
        and tokens.shape[1] == GROUPS * GROUP_DIM
        and out_weight.shape[1] == count * HALF
    )
    if fits:
        return kernel_body(count, tokens, out_weight)
    return general_body(tokens, out_weight)


def solution(mesh):
    placed = (P("row", None), P(None, "col"))
    return jax.shard_map(
        body, mesh=mesh, in_specs=placed, out_specs=P("row", "col"), check_vma=False
    )
```

```python
import math

import functools

import jax
import jax.numpy as jnp
import numpy as np
from jax import lax
from jax.experimental import pallas as pl
from jax.experimental.pallas import tpu as pltpu
from jax.sharding import PartitionSpec as P

GROUPS = 4
GROUP_DIM = 512


def angles(product, period):
    return (product % period).astype(jnp.float32) * (2.0 * math.pi / period)


def plain_dot(matrix, values):
    return jnp.dot(
        matrix, values, precision=lax.Precision.HIGHEST, preferred_element_type=jnp.float32
    )


def whole_transform(whole_rows, row_count, seg_rows, length):
    few_chans = whole_rows.shape[2]
    lattice = jnp.arange(row_count, dtype=jnp.int32)
    phases = angles(lattice[:, None] * lattice[None, :], row_count)
    cosine_table = jnp.cos(phases)
    sine_table = jnp.sin(phases)
    real_in = whole_rows[0].reshape(row_count, seg_rows * few_chans)
    imag_in = whole_rows[1].reshape(row_count, seg_rows * few_chans)
    first_re = (plain_dot(cosine_table, real_in) + plain_dot(sine_table, imag_in)).reshape(
        row_count, seg_rows, few_chans
    )
    first_im = (plain_dot(cosine_table, imag_in) - plain_dot(sine_table, real_in)).reshape(
        row_count, seg_rows, few_chans
    )
    inner = jnp.arange(seg_rows, dtype=jnp.int32)
    twist = angles(lattice[:, None] * inner[None, :], length)[:, :, None]
    twist_cos = jnp.cos(twist)
    twist_sin = jnp.sin(twist)
    turned_re = twist_cos * first_re + twist_sin * first_im
    turned_im = twist_cos * first_im - twist_sin * first_re
    folded_re = jnp.transpose(turned_re, (1, 0, 2)).reshape(seg_rows, row_count * few_chans)
    folded_im = jnp.transpose(turned_im, (1, 0, 2)).reshape(seg_rows, row_count * few_chans)
    seg_phases = angles(inner[:, None] * inner[None, :], seg_rows)
    real_part = plain_dot(jnp.cos(seg_phases), folded_re) + plain_dot(
        jnp.sin(seg_phases), folded_im
    )
    return real_part.reshape(length, few_chans)


def general_body(tokens, out_weight):
    seg_rows = tokens.shape[0]
    col_width = out_weight.shape[1]
    row_count = lax.axis_size("row")
    length = seg_rows * row_count
    scaling = 1.0 / math.sqrt(length * GROUP_DIM)
    weight_wide = out_weight.astype(jnp.float32)
    lattice = jnp.arange(GROUP_DIM, dtype=jnp.int32)
    phases = angles(lattice[:, None] * lattice[None, :], GROUP_DIM)
    cosine_table = jnp.cos(phases) * scaling
    sine_table = jnp.sin(phases) * scaling
    folded_rows = []
    for group in range(GROUPS):
        group_rows = weight_wide[group * GROUP_DIM : (group + 1) * GROUP_DIM]
        folded_rows.append(
            jnp.concatenate(
                [plain_dot(cosine_table, group_rows), -plain_dot(sine_table, group_rows)], axis=1
            )
        )
    folded_map = jnp.concatenate(folded_rows, axis=0)
    spectrum = plain_dot(tokens.astype(jnp.float32), folded_map)
    stacked = jnp.stack([spectrum[:, :col_width], spectrum[:, col_width:]])
    whole_rows = lax.all_to_all(stacked, "row", split_axis=2, concat_axis=1, tiled=True)
    ordered = whole_transform(whole_rows, row_count, seg_rows, length)
    spectral = lax.all_to_all(
        ordered.astype(jnp.bfloat16), "row", split_axis=0, concat_axis=1, tiled=True
    )
    return spectral

RADIX = 8
HALF = 64
LANES = 128
EXTRA = 16
PARTS = 4
CODE = 84.0


def split_table(values):
    big = values.astype(jnp.bfloat16)
    return big, (values - big.astype(np.float64)).astype(jnp.bfloat16)


def tables(size, length):
    index = np.arange(size)
    phase = 2.0 * np.pi * ((index[:, None] * index[None, :]) % size) / size
    high, low = split_table(np.concatenate([np.cos(phase), np.sin(phase)], axis=0))
    turn = 2.0 * np.pi * (index[:, None] * np.arange(RADIX)[None, :]) / length
    twist = np.zeros((size, LANES), np.float32)
    twist[:, :RADIX] = np.cos(turn)
    twist[:, RADIX : 2 * RADIX] = np.sin(turn)
    small = np.arange(RADIX)
    eight = 2.0 * np.pi * ((small[:, None] * small[None, :]) % RADIX) / RADIX
    last = np.concatenate(
        [
            np.repeat(np.cos(eight)[:, :, None], HALF, axis=2),
            np.repeat(np.sin(eight)[:, :, None], HALF, axis=2),
        ],
        axis=2,
    ).astype(np.float32)
    return high, low, twist, last


def dot(a, b):
    return jnp.dot(a, b, preferred_element_type=jnp.float32)


def split(values):
    high = values.astype(jnp.bfloat16)
    return high, (values - high.astype(jnp.float32)).astype(jnp.bfloat16)


def peer_at(step, chip):
    upper = chip // 2
    folded = chip + upper * (3 - 2 * chip)
    place = lax.rem(step + 1 + folded, 4)
    goal = place + place // 2 - 2 * (place // 3)
    return goal + upper * (3 - 2 * goal)


def kernel(
    scaling,
    count,
    tok_hbm,
    w_hbm,
    high_hbm,
    low_hbm,
    twist_ref,
    last_ref,
    out_ref,
    tok_ref,
    w_ref,
    high_ref,
    low_ref,
    tok_s,
    send_a,
    recv_a,
    zhigh,
    zlow,
    turned,
    found_s,
    fold_high,
    fold_low,
    send_b,
    recv_b,
    load_sem,
    send_a_sem,
    recv_a_sem,
    send_b_sem,
    recv_b_sem,
):
    me = lax.axis_index("row")
    chip = me // 2
    chips = count // 2
    size = tok_ref.shape[0]
    groups = tok_ref.shape[1] // size
    inner = size // RADIX
    mid = size // 2
    part_rows = size // PARTS
    loads = []
    for at, (source, target) in enumerate(
        [(high_hbm, high_ref), (low_hbm, low_ref), (tok_hbm, tok_ref)]
    ):
        loads.append(pltpu.make_async_copy(source, target, load_sem.at[at]))

    def load_w(step):
        goal = peer_at(step, chip)
        cols = pl.ds(pl.multiple_of(goal * LANES, LANES), LANES)
        return pltpu.make_async_copy(
            w_hbm.at[:, cols], w_ref.at[:, cols], load_sem.at[3 + step]
        )

    load_w(0).start()
    for load in loads:
        load.start()
    for step in range(1, 4):
        load_w(step).start()
    barrier = pltpu.get_barrier_semaphore()
    for ahead in range(1, count):
        pl.semaphore_signal(
            barrier,
            inc=1,
            device_id={"row": lax.rem(me + ahead, count)},
            device_id_type=pl.DeviceIdType.MESH,
        )

    lane = lax.broadcasted_iota(jnp.int32, (1, LANES), 1)
    first = lane < HALF
    sign = jnp.where(first, 1.0, -1.0)

    def copy_a(part, target):
        return pltpu.make_async_remote_copy(
            src_ref=send_a.at[part, target],
            dst_ref=recv_a.at[part, me],
            send_sem=send_a_sem.at[part, target],
            recv_sem=recv_a_sem.at[part, me],
            device_id={"row": target},
            device_id_type=pl.DeviceIdType.MESH,
        )

    def copy_b(target):
        return pltpu.make_async_remote_copy(
            src_ref=send_b.at[target],
            dst_ref=recv_b.at[me],
            send_sem=send_b_sem.at[target],
            recv_sem=recv_b_sem.at[me],
            device_id={"row": target},
            device_id_type=pl.DeviceIdType.MESH,
        )

    for load in loads[:2]:
        load.wait()

    @pl.loop(0, chips)
    def _(step):
        goal = peer_at(step, chip)
        cols = pl.ds(pl.multiple_of(goal * LANES, LANES), LANES)
        load_w(step).wait()
        side = jnp.concatenate(
            [w_ref[g * size : (g + 1) * size, cols] for g in range(groups)], axis=1
        )
        folded = dot(high_ref[...], side) + dot(low_ref[...], side)

        @pl.when(step == 0)
        def _():
            loads[2].wait()
            place = lax.broadcasted_iota(jnp.int32, (1, size), 1)
            place = (place % RADIX) * inner + place // RADIX
            spot = lax.broadcasted_iota(jnp.int32, (size, size), 0)
            perm = jnp.where(spot == place, 1.0, 0.0).astype(jnp.bfloat16)
            for g in range(groups):
                span = slice(g * size, (g + 1) * size)
                tok_s[:, span] = dot(perm, tok_ref[:, span]).astype(jnp.bfloat16)

        for g in range(groups):
            cosw = folded[:size, g * LANES : (g + 1) * LANES]
            sinw = -folded[size:, g * LANES : (g + 1) * LANES]
            pair = jnp.concatenate(
                [
                    jnp.where(first, cosw, pltpu.roll(sinw, HALF, 1)),
                    jnp.where(first, pltpu.roll(cosw, HALF, 1), sinw),
                ],
                axis=1,
            )
            high, low = split(pair)
            fold_high[g * size : (g + 1) * size] = high
            fold_low[g * size : (g + 1) * size] = low
        total = dot(tok_s[...], fold_high[...]) + dot(tok_s[...], fold_low[...])
        for core in range(2):
            target = goal * 2 + core
            block = total[:, core * LANES : (core + 1) * LANES]
            peak = jnp.max(jnp.abs(block), axis=1, keepdims=True)
            peak = jnp.max(peak, axis=0, keepdims=True)
            scale = jnp.broadcast_to(jnp.maximum(peak, 1e-30) * 1.0079, (EXTRA, LANES))
            scale = scale.astype(jnp.bfloat16)
            factor = CODE / scale[0:1].astype(jnp.float32)
            code = jnp.exp(jnp.abs(block) * factor) - 1.0
            code = jnp.where(block < 0.0, -code, code).astype(jnp.bfloat16)
            for part in range(PARTS):
                rows = slice(part * part_rows, (part + 1) * part_rows)
                send_a[part, target, :part_rows] = code[rows]
                send_a[part, target, part_rows:] = scale

        def ship(parts, steps):
            for part in parts:
                for at in steps:
                    for core in range(2):
                        copy_a(part, peer_at(at, chip) * 2 + core).start()

        half = range(PARTS // 2)
        rest = range(PARTS // 2, PARTS)

        @pl.when(step == 0)
        def _():
            pl.semaphore_wait(barrier, count - 1)
            ship(half, [0])

        @pl.when(step == 1)
        def _():
            ship(half, [1])
            ship(range(PARTS // 2, PARTS - 1), [0, 1])

        @pl.when(step == 2)
        def _():
            ship(half, [2])
            ship(range(PARTS // 2, PARTS - 1), [2])
            ship(range(PARTS - 1, PARTS), [0, 1, 2])

        @pl.when(step == chips - 1)
        def _():
            for part in range(PARTS):
                copy_a(part, chip * 2 + (1 - me % 2)).start()
                recv_a[part, me] = send_a[part, me]

    for pair in range(RADIX // 2):

        def take(at, base):
            source = base + at

            @pl.when(source != me)
            def _():
                pltpu.make_async_remote_copy(
                    src_ref=send_a.at[pair, source],
                    dst_ref=recv_a.at[pair, source],
                    send_sem=send_a_sem.at[pair, source],
                    recv_sem=recv_a_sem.at[pair, source],
                    device_id={"row": source},
                    device_id_type=pl.DeviceIdType.MESH,
                ).wait_recv()

            factor = recv_a[pair, source, part_rows:].astype(jnp.float32)[0:1]
            factor = factor * (scaling / CODE)
            code = recv_a[pair, source, :part_rows].astype(jnp.float32)
            value = jnp.log(1.0 + jnp.abs(code)) * factor
            value = jnp.where(code < 0.0, -value, value)
            high, low = split(value)
            rows = pl.ds(pl.multiple_of(source * inner, inner), inner)
            for half in range(2):
                span = slice((pair * 2 + half) * LANES, (pair * 2 + half + 1) * LANES)
                zhigh[rows, span] = high[half * inner : (half + 1) * inner]
                zlow[rows, span] = low[half * inner : (half + 1) * inner]

        def near_or_far(base):
            pl.loop(0, count // 2)(lambda at: take(at, base))
            span = pl.ds(pl.multiple_of(base * inner, size // 2), size // 2)
            terms = dot(high_ref[:, span], zhigh[span, cols])
            terms += dot(high_ref[:, span], zlow[span, cols])
            return terms + dot(low_ref[:, span], zhigh[span, cols])

        cols = slice(pair * 2 * LANES, (pair + 1) * 2 * LANES)
        own = (me // (count // 2)) * (count // 2)
        found_s[...] = near_or_far(own)
        found = found_s[...] + near_or_far(count // 2 - own)
        for half in range(2):
            t = pair * 2 + half
            cosz = found[:size, half * LANES : (half + 1) * LANES]
            sinz = found[size:, half * LANES : (half + 1) * LANES]
            whole = cosz + sign * pltpu.roll(sinz, HALF, 1)
            if t:
                whole = twist_ref[:, t : t + 1] * whole + (
                    twist_ref[:, RADIX + t : RADIX + t + 1] * sign
                ) * pltpu.roll(whole, HALF, 1)
            turned[t] = whole

    @pl.loop(0, count)
    def _(at):
        target = peer_at(at // 2, chip) * 2 + at % 2
        weights = last_ref[target]
        rows_at = 32
        for chunk in range(mid // rows_at):
            upper = slice(chunk * rows_at, (chunk + 1) * rows_at)
            under = slice(mid + chunk * rows_at, mid + (chunk + 1) * rows_at)
            top = weights[0:1] * turned[0, upper]
            bottom = weights[0:1] * turned[0, under]
            for t in range(1, RADIX):
                top += weights[t : t + 1] * turned[t, upper]
                bottom += weights[t : t + 1] * turned[t, under]
            packed = jnp.where(first, top, bottom) + pltpu.roll(
                jnp.where(first, bottom, top), HALF, 1
            )
            packed = packed.astype(jnp.bfloat16)
            send_b[target, upper] = packed

        @pl.when(target != me)
        def _():
            copy_b(target).start()

    recv_b[me] = send_b[me]

    for at in range(chips):
        goal = peer_at(chips - 1 - at, chip)
        for core in range(2):
            source = goal * 2 + core

            @pl.when(source != me)
            def _():
                pltpu.make_async_remote_copy(
                    src_ref=send_b.at[source],
                    dst_ref=recv_b.at[source],
                    send_sem=send_b_sem.at[source],
                    recv_sem=recv_b_sem.at[source],
                    device_id={"row": source},
                    device_id_type=pl.DeviceIdType.MESH,
                ).wait_recv()

        left = recv_b[goal * 2].astype(jnp.float32)
        right = recv_b[goal * 2 + 1].astype(jnp.float32)
        cols = pl.ds(pl.multiple_of(goal * LANES, LANES), LANES)
        out_ref[:mid, cols] = jnp.where(first, left, pltpu.roll(right, HALF, 1)).astype(
            jnp.bfloat16
        )
        out_ref[mid:, cols] = jnp.where(first, pltpu.roll(left, HALF, 1), right).astype(
            jnp.bfloat16
        )

    @pl.loop(1, count)
    def _(ahead):
        target = lax.rem(me + ahead, count)
        for part in range(PARTS):
            copy_a(part, target).wait_send()
        copy_b(target).wait_send()


def kernel_body(count, tokens, out_weight):
    size = tokens.shape[0]
    length = size * count
    scaling = 1.0 / math.sqrt(length * GROUP_DIM)
    vmem = pl.BlockSpec(memory_space=pltpu.VMEM)
    consts = [jnp.asarray(table) for table in tables(size, length)]
    return pl.pallas_call(
        functools.partial(kernel, scaling, count),
        out_shape=jax.ShapeDtypeStruct((size, out_weight.shape[1]), jnp.bfloat16),
        in_specs=[pl.BlockSpec(memory_space=pl.ANY)] * 4 + [vmem] * 2,
        out_specs=vmem,
        scratch_shapes=[
            pltpu.VMEM(tokens.shape, jnp.bfloat16),
            pltpu.VMEM(out_weight.shape, jnp.bfloat16),
            pltpu.VMEM((2 * size, size), jnp.bfloat16),
            pltpu.VMEM((2 * size, size), jnp.bfloat16),
            pltpu.VMEM(tokens.shape, jnp.bfloat16),
            pltpu.VMEM((PARTS, count, size // PARTS + EXTRA, LANES), jnp.bfloat16),
            pltpu.VMEM((PARTS, count, size // PARTS + EXTRA, LANES), jnp.bfloat16),
            pltpu.VMEM((size, RADIX * LANES), jnp.bfloat16),
            pltpu.VMEM((size, RADIX * LANES), jnp.bfloat16),
            pltpu.VMEM((RADIX, size, LANES), jnp.float32),
            pltpu.VMEM((2 * size, 2 * LANES), jnp.float32),
            pltpu.VMEM((tokens.shape[1], 2 * LANES), jnp.bfloat16),
            pltpu.VMEM((tokens.shape[1], 2 * LANES), jnp.bfloat16),
            pltpu.VMEM((count, size // 2, LANES), jnp.bfloat16),
            pltpu.VMEM((count, size // 2, LANES), jnp.bfloat16),
            pltpu.SemaphoreType.DMA((7,)),
            pltpu.SemaphoreType.DMA((PARTS, count)),
            pltpu.SemaphoreType.DMA((PARTS, count)),
            pltpu.SemaphoreType.DMA((count,)),
            pltpu.SemaphoreType.DMA((count,)),
        ],
        compiler_params=pltpu.CompilerParams(
            collective_id=0, has_side_effects=True, vmem_limit_bytes=60 * 1024 * 1024
        ),
    )(tokens, out_weight, *consts)


def body(tokens, out_weight):
    size = tokens.shape[0]
    count = lax.axis_size("row")
    fits = (
        count == RADIX
        and size == GROUP_DIM
        and tokens.shape[1] == GROUPS * GROUP_DIM
        and out_weight.shape[1] == count * HALF
    )
    if fits:
        return kernel_body(count, tokens, out_weight)
    return general_body(tokens, out_weight)


def solution(mesh):
    placed = (P("row", None), P(None, "col"))
    return jax.shard_map(
        body, mesh=mesh, in_specs=placed, out_specs=P("row", "col"), check_vma=False
    )
```
